32 devices in a mesh: gr: 2 (over y), sp: 4 (over z), tp: 4 (over x, core).
Axes of the slice: x: 2, y: 2, z: 4, core: 2. Of those that a mesh axis runs over, the one named last changes fastest.
Arguments:
- layer_input: bfloat16 [2, 3072, 2048], P('gr', ('sp', 'tp')), may hold values from -6 to 6
- key_weight: bfloat16 [2048, 2048], P(None, 'tp'), may hold values from -0.125 to 0.125
- value_weight: bfloat16 [2048, 2048], P(None, 'tp'), may hold values from -0.125 to 0.125
- new_queries: bfloat16 [2, 2048], P('gr', 'tp'), may hold values from -280 to 280
- lambdas: float32 [16], P('tp'), may hold values from 0.3 to 0.8
- head_gain: float32 [128], replicated, may hold values from 0.1 to 1.9
- out_weight: bfloat16 [2048, 2048], P('tp'), may hold values from -0.125 to 0.125
Outputs:
- key_cache: bfloat16 [2, 3072, 2048], P('gr', 'sp', 'tp')
- value_cache: bfloat16 [2, 3072, 2048], P('gr', 'sp', 'tp')
- mixed: bfloat16 [2, 2048], P('gr', 'tp')
The draws below stay inside these ranges and needn't reach their ends.
All inputs are finite; a program needn't handle non-finite values.
Results may differ from the reference program's by a relative error of at most 0.03.
Values may be sent and summed in bfloat16 or wider, within the bound.
A program may use at most 64 MiB of HBM per device.

```python
import jax
import jax.numpy as jnp
from jax import lax

D = 2048
HEADS = 16
HEAD_DIM = 64
ROWS = 192
LEN = 3072
SEQS = 2
N_SP = 4
N_TP = 4


def draw_new_queries(key, part):
    drawn_rows = jax.random.normal(jax.random.fold_in(key, 11), (SEQS, HEADS * 2 * HEAD_DIM), jnp.float32)
    drawn_rows = jnp.clip(drawn_rows, -4.0, 4.0) * 1.7
    return drawn_rows.astype(jnp.bfloat16)


def block_scale(key, shape, pieces, low, high):
    factor_of, own = 1.0, jax.random.fold_in(key, 6)
    for position, parts in pieces:
        heights = jnp.exp(jax.random.uniform(jax.random.fold_in(own, position), (parts,), jnp.float32, low / len(pieces), high / len(pieces)))
        factor_of = factor_of * jnp.repeat(heights, shape[position] // parts).reshape([-1 if axis == position else 1 for axis in range(len(shape))])
    return factor_of


def gaussian(own_key, dims, scale, most, cuts=(), kind=jnp.bfloat16):
    loudness = block_scale(own_key, dims, cuts, -0.22, 0.18) if cuts else 1.0
    entries = jax.random.normal(own_key, dims, jnp.float32) * scale * loudness
    return jnp.minimum(jnp.maximum(entries, -most), most).astype(kind)


def setup_inputs(seed: int = 0) -> dict:
    arg_keys = jax.random.split(jax.random.key(seed), 8)
    return {
        "layer_input": gaussian(arg_keys[0], (SEQS, LEN, D), 1.0, 6.0, ((0, 2), (1, 16))),
        "key_weight": gaussian(arg_keys[1], (D, HEADS * 2 * HEAD_DIM), D ** -0.5, 0.125, ((1, 4),)),
        "value_weight": gaussian(arg_keys[2], (D, HEADS * 2 * HEAD_DIM), D ** -0.5, 0.125, ((1, 4),)),
        "new_queries": draw_new_queries(jax.random.fold_in(arg_keys[7], 71), 0),
        "lambdas": jnp.clip(0.3 + 0.5 * jax.random.uniform(arg_keys[4], (HEADS,), jnp.float32) ** block_scale(arg_keys[4], (HEADS,), ((0, 4),), -0.2, 0.2), 0.3, 0.8),
        "head_gain": jnp.clip(1.0 + 0.18 * jax.random.normal(arg_keys[5], (2 * HEAD_DIM,), jnp.float32), 0.1, 1.9),
        "out_weight": gaussian(arg_keys[6], (HEADS * 2 * HEAD_DIM, D), (HEADS * 2 * HEAD_DIM) ** -0.5, 0.125, ((0, 4),)),
    }


def rotate(raw_keys, positions, head_dim):
    inverse = 1.0 / 10000.0 ** (jnp.arange(0, head_dim, 2, dtype=jnp.float32) / head_dim)
    angles = positions.astype(jnp.float32)[:, None] * inverse[None, :]
    angles = jnp.concatenate([angles, angles], axis=-1)
    cosine = jnp.cos(angles)[:, None, :]
    sine = jnp.sin(angles)[:, None, :]
    first_half, second_half = jnp.split(raw_keys, 2, axis=-1)
    turned = jnp.concatenate([-second_half, first_half], axis=-1)
    return raw_keys * cosine + turned * sine

def reference(layer_input, key_weight, value_weight, new_queries, lambdas, head_gain, out_weight):
    block_rows = ROWS * N_TP
    column_count = HEADS * 2 * HEAD_DIM

    def project(items):
        block, index = items
        raw_keys = jnp.dot(block, key_weight, preferred_element_type=jnp.float32)
        raw_keys = raw_keys.reshape(block_rows, 2 * HEADS, HEAD_DIM)
        positions = index * block_rows + jnp.arange(block_rows, dtype=jnp.int32)
        key_rows = rotate(raw_keys, positions, HEAD_DIM)
        key_rows = key_rows.reshape(block_rows, column_count).astype(jnp.bfloat16)
        value_rows = jnp.dot(block, value_weight, preferred_element_type=jnp.float32).astype(jnp.bfloat16)
        return (key_rows, value_rows)
    key_list = []
    value_list = []
    read_list = []
    for seq_index in range(SEQS):
        blocks = layer_input[seq_index].reshape(N_SP, block_rows, D)
        key_blocks, value_blocks = lax.map(project, (blocks, jnp.arange(N_SP, dtype=jnp.int32)))
        key_rows = key_blocks.reshape(LEN, column_count)
        value_rows = value_blocks.reshape(LEN, column_count)
        query_row = new_queries[seq_index].astype(jnp.float32)

        def read_head(head):
            first = (head * 2 * HEAD_DIM).astype(jnp.int32)
            key_part = lax.dynamic_slice_in_dim(key_rows, first, 2 * HEAD_DIM, 1).astype(jnp.float32)
            key_part = key_part.reshape(LEN, 2, HEAD_DIM)
            value_part = lax.dynamic_slice_in_dim(value_rows, first, 2 * HEAD_DIM, 1).astype(jnp.float32)
            query_part = lax.dynamic_slice_in_dim(query_row, first, 2 * HEAD_DIM, 0).reshape(2, HEAD_DIM)
            scores = jnp.einsum('md,lmd->ml', query_part, key_part) * HEAD_DIM ** (-0.5)
            maps = jax.nn.softmax(scores, axis=-1)
            return jnp.einsum('ml,le->me', maps, value_part)
        read_list.append(lax.map(read_head, jnp.arange(HEADS, dtype=jnp.int32)))
        key_list.append(key_rows)
        value_list.append(value_rows)
    key_cache = jnp.stack(key_list, axis=0)
    value_cache = jnp.stack(value_list, axis=0)
    reads = jnp.stack(read_list, axis=0)
    diff = reads[:, :, 0] - lambdas[None, :, None] * reads[:, :, 1]
    normed = diff * lax.rsqrt(lax.optimization_barrier(jnp.mean(diff * diff, axis=-1, keepdims=True)) + 1e-06) * head_gain
    headed = normed.reshape(SEQS, column_count).astype(jnp.bfloat16)
    group_cols = column_count // N_TP
    grouped = headed.reshape(SEQS, N_TP, group_cols).astype(jnp.float32)
    weight_groups = out_weight.reshape(N_TP, group_cols, D).astype(jnp.float32)
    partials = jnp.einsum('stc,tcd->std', grouped, weight_groups).astype(jnp.bfloat16)
    mixed = lax.optimization_barrier(jnp.sum(partials.astype(jnp.float32), axis=1)).astype(jnp.bfloat16)
    return (key_cache, value_cache, mixed)
```

```python
import functools

import jax
import jax.numpy as jnp
import numpy as np
from jax import lax
from jax.experimental import pallas as pl
from jax.experimental.pallas import tpu as pltpu
from jax.sharding import PartitionSpec as P

MESH = pl.DeviceIdType.MESH
MAP_ROWS = 16


def kernel(
    n_sp, n_tp, heads, head_dim, chunk,
    x_ref, wk_ref, wv_ref, q_ref, lam_ref, gain_ref, wo_ref, fine_ref, coarse_ref,
    k_ref, v_ref, mix_ref,
    xg, wk, wv, wo, q, lam, gain, fine, coarse, keys, values, stats, part, parts,
    load_sem, out_sem, near_send, near_recv, far_send, far_recv, fwd_send, fwd_recv,
    st_send, st_recv, pt_send, pt_recv,
):
    sp = lax.axis_index("sp")
    tp = lax.axis_index("tp")
    rows = x_ref.shape[1]
    wide = 2 * head_dim
    maps = 2 * heads
    steps = rows // chunk
    chips = n_tp // 2
    partner = tp + 1 - 2 * lax.rem(tp, 2)
    out_cols = mix_ref.shape[1]
    local_coarse = n_tp * steps

    loads = [
        pltpu.make_async_copy(x_ref.at[0], xg.at[tp], load_sem.at[0]),
        pltpu.make_async_copy(wk_ref, wk, load_sem.at[1]),
        pltpu.make_async_copy(wv_ref, wv, load_sem.at[2]),
        pltpu.make_async_copy(fine_ref, fine, load_sem.at[3]),
        pltpu.make_async_copy(
            coarse_ref.at[pl.ds(sp * local_coarse, local_coarse)], coarse, load_sem.at[4]
        ),
        pltpu.make_async_copy(q_ref, q, load_sem.at[5]),
        pltpu.make_async_copy(lam_ref, lam, load_sem.at[6]),
        pltpu.make_async_copy(gain_ref, gain, load_sem.at[7]),
        pltpu.make_async_copy(wo_ref, wo, load_sem.at[8]),
    ]

    barrier = pltpu.get_barrier_semaphore()
    for d in range(1, n_tp):
        pl.semaphore_signal(
            barrier, inc=1, device_id={"tp": lax.rem(tp + d, n_tp)}, device_id_type=MESH
        )
    for d in range(1, n_sp):
        pl.semaphore_signal(
            barrier, inc=1, device_id={"sp": lax.rem(sp + d, n_sp)}, device_id_type=MESH
        )
    for load in loads:
        load.start()
    pl.semaphore_wait(barrier, n_tp - 1 + n_sp - 1)

    far = {}
    for j in range(steps):
        for d in range(1, chips):
            far[d, j] = pltpu.make_async_remote_copy(
                src_ref=x_ref.at[0, pl.ds(j * chunk, chunk)],
                dst_ref=xg.at[tp, pl.ds(j * chunk, chunk)],
                send_sem=far_send.at[d - 1, j],
                recv_sem=far_recv.at[d - 1, j],
                device_id={"tp": lax.rem(tp + 2 * d, n_tp)},
                device_id_type=MESH,
            )
            far[d, j].start()
    near = pltpu.make_async_remote_copy(
        src_ref=x_ref.at[0],
        dst_ref=xg.at[tp],
        send_sem=near_send,
        recv_sem=near_recv,
        device_id={"tp": partner},
        device_id_type=MESH,
    )
    near.start()

    lane = lax.broadcasted_iota(jnp.int32, (chunk, wide), 1)
    low_half = lax.rem(lane, head_dim) < head_dim // 2

    def project(block, first, count):
        piece = xg[block, first * chunk:(first + count) * chunk, :]
        raw_keys = jnp.dot(piece, wk[...], preferred_element_type=jnp.float32)
        raw_values = jnp.dot(piece, wv[...], preferred_element_type=jnp.float32)
        values[block, first * chunk:(first + count) * chunk, :] = raw_values.astype(jnp.bfloat16)
        for i in range(count):
            base = coarse[block * steps + first + i]
            base_cos, base_sin = base[0:1, :], base[1:2, :]
            cosine = base_cos * fine[0] - base_sin * fine[1]
            sine = base_sin * fine[0] + base_cos * fine[1]
            for h in range(heads):
                raw = raw_keys[i * chunk:(i + 1) * chunk, h * wide:(h + 1) * wide]
                ahead = pltpu.roll(raw, wide - head_dim // 2, 1)
                behind = pltpu.roll(raw, head_dim // 2, 1)
                turned = raw * cosine + jnp.where(low_half, ahead, behind) * sine
                keys[
                    block, (first + i) * chunk:(first + i + 1) * chunk, h * wide:(h + 1) * wide
                ] = turned.astype(jnp.bfloat16)

    outs = []

    def put(block, first, count, slot):
        where = pl.ds(first * chunk, count * chunk)
        for held, ref, s in ((keys, k_ref, 0), (values, v_ref, 1)):
            copy = pltpu.make_async_copy(
                held.at[block, where], ref.at[block, where], out_sem.at[s, slot]
            )
            copy.start()
            outs.append(copy)

    for load in loads[:5]:
        load.wait()
    project(tp, 0, steps)
    put(tp, 0, steps, 0)
    near.wait_recv()
    project(partner, 0, steps)
    put(partner, 0, steps, 1)

    forwards = []
    slot = 2
    for j in range(steps):
        for d in range(1, chips):
            source = lax.rem(tp + n_tp - 2 * d, n_tp)
            other = source + 1 - 2 * lax.rem(source, 2)
            far[d, j].wait_recv()
            forward = pltpu.make_async_remote_copy(
                src_ref=xg.at[source, pl.ds(j * chunk, chunk)],
                dst_ref=xg.at[source, pl.ds(j * chunk, chunk)],
                send_sem=fwd_send.at[d - 1, j],
                recv_sem=fwd_recv.at[d - 1, j],
                device_id={"tp": partner},
                device_id_type=MESH,
            )
            forward.start()
            forwards.append(forward)
            project(source, j, 1)
            put(source, j, 1, slot)
            forward.wait_recv()
            project(other, j, 1)
            put(other, j, 1, slot + 1)
            slot += 2

    for load in loads[5:]:
        load.wait()
    map_row = lax.broadcasted_iota(jnp.int32, (MAP_ROWS, q.shape[1]), 0)
    map_col = lax.broadcasted_iota(jnp.int32, (MAP_ROWS, q.shape[1]), 1) // head_dim
    spread = jnp.where(map_row == map_col, q[...].astype(jnp.float32), 0.0).astype(jnp.bfloat16)
    scores = [
        lax.dot_general(
            spread, keys[b], (((1,), (1,)), ((), ())), preferred_element_type=jnp.float32
        ) * head_dim ** (-0.5)
        for b in range(n_tp)
    ]
    highest = functools.reduce(
        jnp.maximum, [jnp.max(s, axis=1, keepdims=True) for s in scores]
    )
    total = jnp.zeros_like(highest)
    read = jnp.zeros((MAP_ROWS, q.shape[1]), jnp.float32)
    for b in range(n_tp):
        weight = jnp.exp(scores[b] - highest)
        total = total + jnp.sum(weight, axis=1, keepdims=True)
        upper = weight.astype(jnp.bfloat16)
        lower = (weight - upper.astype(jnp.float32)).astype(jnp.bfloat16)
        read = read + jnp.dot(upper, values[b], preferred_element_type=jnp.float32)
        read = read + jnp.dot(lower, values[b], preferred_element_type=jnp.float32)
    head_of = lax.broadcasted_iota(jnp.int32, (MAP_ROWS, wide), 0) // 2
    own = jnp.zeros((MAP_ROWS, wide), jnp.float32)
    for h in range(heads):
        own = jnp.where(head_of == h, read[:, h * wide:(h + 1) * wide], own)
    first_lane = lax.broadcasted_iota(jnp.int32, (MAP_ROWS, wide), 1) == 0
    stats[sp, 0] = own[:maps]
    stats[sp, 1] = jnp.where(first_lane, highest, total)[:maps]

    exchanges = []
    for d in range(n_sp - 1, 0, -1):
        copy = pltpu.make_async_remote_copy(
            src_ref=stats.at[sp],
            dst_ref=stats.at[sp],
            send_sem=st_send.at[d - 1],
            recv_sem=st_recv.at[d - 1],
            device_id={"sp": lax.rem(sp + d, n_sp)},
            device_id_type=MESH,
        )
        copy.start()
        exchanges.append(copy)
    for copy in exchanges:
        copy.wait_recv()
    heights = stats[:, 1]
    tops = heights[:, :, 0:1]
    sums = heights[:, :, 1:2]
    factor = jnp.exp(tops - jnp.max(tops, axis=0, keepdims=True))
    totals = jnp.sum(sums * factor, axis=0)
    reads = jnp.sum(stats[:, 0] * factor, axis=0) / totals
    normed = []
    for h in range(heads):
        diff = reads[2 * h:2 * h + 1] - lam[0:1, h:h + 1] * reads[2 * h + 1:2 * h + 2]
        scale = lax.rsqrt(jnp.mean(diff * diff, axis=1, keepdims=True) + 1e-06)
        normed.append(diff * scale * gain[...])
    headed = jnp.concatenate(normed, axis=1)
    headed = jnp.broadcast_to(headed, (MAP_ROWS, headed.shape[1])).astype(jnp.bfloat16)
    partials = jnp.dot(headed, wo[...], preferred_element_type=jnp.float32).astype(jnp.bfloat16)
    for b in range(n_tp):
        part[b] = partials[:, b * out_cols:(b + 1) * out_cols]
    swaps = []
    for d in range(n_tp - 1, 0, -1):
        target = lax.rem(tp + d, n_tp)
        copy = pltpu.make_async_remote_copy(
            src_ref=part.at[target],
            dst_ref=parts.at[d - 1],
            send_sem=pt_send.at[d - 1],
            recv_sem=pt_recv.at[d - 1],
            device_id={"tp": target},
            device_id_type=MESH,
        )
        copy.start()
        swaps.append(copy)
    mixed = part[tp].astype(jnp.float32)
    for copy in swaps:
        copy.wait_recv()
    for d in range(1, n_tp):
        mixed = mixed + parts[d - 1].astype(jnp.float32)
    mix_ref[...] = mixed[0:1].astype(jnp.bfloat16)

    near.wait_send()
    for copy in list(far.values()) + forwards + exchanges + swaps:
        copy.wait_send()
    for copy in outs:
        copy.wait()


def tables(length, chunk, head_dim):
    inverse = 1.0 / 10000.0 ** (np.arange(0, head_dim, 2) / head_dim)
    inverse = np.tile(inverse, 4)
    sign = np.tile(np.repeat([-1.0, 1.0], head_dim // 2), 2)

    def pair(positions, axis):
        angles = positions[:, None] * inverse[None, :]
        both = np.stack([np.cos(angles), np.sin(angles) * sign], axis=axis)
        return both.astype(np.float32)

    return pair(np.arange(chunk), 0), pair(np.arange(0, length, chunk), 1)


def on_device(n_sp, n_tp, x, key_weight, value_weight, new_queries, lambdas, head_gain, out_weight):
    heads = lambdas.shape[0]
    columns = key_weight.shape[1]
    head_dim = columns // (2 * heads)
    wide = 2 * head_dim
    seqs, rows, depth = x.shape
    assert seqs == 1
    chunk = rows // 4
    steps = rows // chunk
    chips = n_tp // 2
    out_cols = out_weight.shape[1] // n_tp
    fine, coarse = tables(n_sp * n_tp * rows, chunk, head_dim)
    any_spec = pl.BlockSpec(memory_space=pl.ANY)
    dma = pltpu.SemaphoreType.DMA
    bf16 = jnp.bfloat16
    f32 = jnp.float32
    slots = 2 + 2 * steps * (chips - 1)
    k, v, mixed = pl.pallas_call(
        functools.partial(kernel, n_sp, n_tp, heads, head_dim, chunk),
        out_shape=(
            jax.ShapeDtypeStruct((n_tp, rows, columns), bf16),
            jax.ShapeDtypeStruct((n_tp, rows, columns), bf16),
            jax.ShapeDtypeStruct((1, out_cols), bf16),
        ),
        in_specs=[any_spec] * 9,
        out_specs=(any_spec, any_spec, pl.BlockSpec(memory_space=pltpu.VMEM)),
        scratch_shapes=[
            pltpu.VMEM((n_tp, rows, depth), bf16),
            pltpu.VMEM((depth, columns), bf16),
            pltpu.VMEM((depth, columns), bf16),
            pltpu.VMEM(out_weight.shape, bf16),
            pltpu.VMEM((1, columns), bf16),
            pltpu.VMEM((1, heads), f32),
            pltpu.VMEM((1, wide), f32),
            pltpu.VMEM((2, chunk, wide), f32),
            pltpu.VMEM((n_tp * steps, 2, wide), f32),
            pltpu.VMEM((n_tp, rows, columns), bf16),
            pltpu.VMEM((n_tp, rows, columns), bf16),
            pltpu.VMEM((n_sp, 2, 2 * heads, wide), f32),
            pltpu.VMEM((n_tp, MAP_ROWS, out_cols), bf16),
            pltpu.VMEM((n_tp - 1, MAP_ROWS, out_cols), bf16),
            dma((9,)),
            dma((2, slots)),
            dma,
            dma,
            dma((chips - 1, steps)),
            dma((chips - 1, steps)),
            dma((chips - 1, steps)),
            dma((chips - 1, steps)),
            dma((n_sp - 1,)),
            dma((n_sp - 1,)),
            dma((n_tp - 1,)),
            dma((n_tp - 1,)),
        ],
        compiler_params=pltpu.CompilerParams(
            collective_id=0, has_side_effects=True, vmem_limit_bytes=60 * 1024 * 1024
        ),
    )(
        x, key_weight, value_weight, new_queries, lambdas.reshape(1, heads),
        head_gain.reshape(1, wide), out_weight, jnp.asarray(fine), jnp.asarray(coarse),
    )
    full = (1, n_tp * rows, columns)
    return k.reshape(full), v.reshape(full), mixed


def solution(mesh):
    n_sp, n_tp = mesh.shape["sp"], mesh.shape["tp"]
    in_specs = (
        P("gr", ("sp", "tp"), None),
        P(None, "tp"),
        P(None, "tp"),
        P("gr", "tp"),
        P("tp"),
        P(),
        P("tp", None),
    )
    out_specs = (P("gr", "sp", "tp"), P("gr", "sp", "tp"), P("gr", "tp"))
    return jax.shard_map(
        functools.partial(on_device, n_sp, n_tp),
        mesh=mesh, in_specs=in_specs, out_specs=out_specs, check_vma=False,
    )
```

```python
import functools

import jax
import jax.numpy as jnp
import numpy as np
from jax import lax
from jax.experimental import pallas as pl
from jax.experimental.pallas import tpu as pltpu
from jax.sharding import PartitionSpec as P

MESH = pl.DeviceIdType.MESH
MAP_ROWS = 16
VMEM_BYTES = 67043328
SMALL_BYTES = 16384


def kernel(
    n_sp, n_tp, heads, head_dim, chunk,
    x_ref, wk_ref, wv_ref, q_ref, lam_ref, gain_ref, wo_ref, fine_ref, coarse_ref,
    keys, values, mix_ref,
    xg, wk, wv, wo, q, lam, gain, fine, coarse, stats, part, parts,
    load_sem, up_sem, down_sem, near_send, near_recv, far_send, far_recv, fwd_send, fwd_recv,
    st_send, st_recv, pt_send, pt_recv,
):
    sp = lax.axis_index("sp")
    tp = lax.axis_index("tp")
    rows = x_ref.shape[1]
    wide = 2 * head_dim
    maps = 2 * heads
    steps = rows // chunk
    chips = n_tp // 2
    partner = tp + 1 - 2 * lax.rem(tp, 2)
    out_cols = mix_ref.shape[1]
    local_coarse = n_tp * steps

    loads = [
        pltpu.make_async_copy(q_ref, q, load_sem.at[5]),
        pltpu.make_async_copy(x_ref.at[0], xg.at[tp], load_sem.at[0]),
        pltpu.make_async_copy(wk_ref, wk, load_sem.at[1]),
        pltpu.make_async_copy(wv_ref, wv, load_sem.at[2]),
        pltpu.make_async_copy(fine_ref, fine, load_sem.at[3]),
        pltpu.make_async_copy(
            coarse_ref.at[pl.ds(sp * local_coarse, local_coarse)], coarse, load_sem.at[4]
        ),
        pltpu.make_async_copy(lam_ref, lam, load_sem.at[6]),
        pltpu.make_async_copy(gain_ref, gain, load_sem.at[7]),
        pltpu.make_async_copy(wo_ref, wo, load_sem.at[8]),
    ]

    barrier = pltpu.get_barrier_semaphore()
    for d in range(1, n_tp):
        pl.semaphore_signal(
            barrier, inc=1, device_id={"tp": lax.rem(tp + d, n_tp)}, device_id_type=MESH
        )
    has_lower = sp > 0
    has_upper = sp < n_sp - 1

    @pl.when(has_lower)
    def _():
        pl.semaphore_signal(barrier, inc=1, device_id={"sp": sp - 1}, device_id_type=MESH)

    @pl.when(has_upper)
    def _():
        pl.semaphore_signal(barrier, inc=1, device_id={"sp": sp + 1}, device_id_type=MESH)

    for load in loads:
        load.start()
    pl.semaphore_wait(barrier, n_tp - 1 + jnp.where(has_lower, 1, 0) + jnp.where(has_upper, 1, 0))

    far = {}
    for j in range(steps):
        for d in range(1, chips):
            far[d, j] = pltpu.make_async_remote_copy(
                src_ref=x_ref.at[0, pl.ds(j * chunk, chunk)],
                dst_ref=xg.at[tp, pl.ds(j * chunk, chunk)],
                send_sem=far_send.at[d - 1, j],
                recv_sem=far_recv.at[d - 1, j],
                device_id={"tp": lax.rem(tp + 2 * d, n_tp)},
                device_id_type=MESH,
            )
            far[d, j].start()
    near = pltpu.make_async_remote_copy(
        src_ref=x_ref.at[0],
        dst_ref=xg.at[tp],
        send_sem=near_send,
        recv_sem=near_recv,
        device_id={"tp": partner},
        device_id_type=MESH,
    )
    near.start()

    pl.when(has_lower)(lambda: pl.semaphore_wait(up_sem, 1))

    @pl.when(has_upper)
    def _():
        pl.semaphore_signal(up_sem, inc=1, device_id={"sp": sp + 1}, device_id_type=MESH)
        pl.semaphore_wait(down_sem, 1)

    @pl.when(has_lower)
    def _():
        pl.semaphore_signal(down_sem, inc=1, device_id={"sp": sp - 1}, device_id_type=MESH)

    lane = lax.broadcasted_iota(jnp.int32, (chunk, wide), 1)
    low_half = lax.rem(lane, head_dim) < head_dim // 2

    def project(block, first, count):
        piece = xg[block, first * chunk:(first + count) * chunk, :]
        raw_keys = jnp.dot(piece, wk[...], preferred_element_type=jnp.float32)
        raw_values = jnp.dot(piece, wv[...], preferred_element_type=jnp.float32)
        values[block, first * chunk:(first + count) * chunk, :] = raw_values.astype(jnp.bfloat16)
        for i in range(count):
            base = coarse[block * steps + first + i]
            base_cos, base_sin = base[0:1, :], base[1:2, :]
            cosine = base_cos * fine[0] - base_sin * fine[1]
            sine = base_sin * fine[0] + base_cos * fine[1]
            for h in range(heads):
                raw = raw_keys[i * chunk:(i + 1) * chunk, h * wide:(h + 1) * wide]
                ahead = pltpu.roll(raw, wide - head_dim // 2, 1)
                behind = pltpu.roll(raw, head_dim // 2, 1)
                turned = raw * cosine + jnp.where(low_half, ahead, behind) * sine
                keys[
                    block, (first + i) * chunk:(first + i + 1) * chunk, h * wide:(h + 1) * wide
                ] = turned.astype(jnp.bfloat16)

    for load in loads[:6]:
        load.wait()
    map_row = lax.broadcasted_iota(jnp.int32, (MAP_ROWS, q.shape[1]), 0)
    map_col = lax.broadcasted_iota(jnp.int32, (MAP_ROWS, q.shape[1]), 1) // head_dim
    spread = jnp.where(map_row == map_col, q[...].astype(jnp.float32), 0.0).astype(jnp.bfloat16)

    def attend(state, block, first, count):
        where = slice(first * chunk, (first + count) * chunk)
        score = lax.dot_general(
            spread, keys[block, where, :], (((1,), (1,)), ((), ())),
            preferred_element_type=jnp.float32,
        ) * head_dim ** (-0.5)
        highest = jnp.max(score, axis=1, keepdims=True)
        if state is not None:
            highest = jnp.maximum(highest, state[0])
        weight = jnp.exp(score - highest)
        total = jnp.sum(weight, axis=1, keepdims=True)
        upper = weight.astype(jnp.bfloat16)
        lower = (weight - upper.astype(jnp.float32)).astype(jnp.bfloat16)
        read = jnp.dot(
            jnp.concatenate([upper, lower], axis=0), values[block, where, :],
            preferred_element_type=jnp.float32,
        )
        read = read[:MAP_ROWS] + read[MAP_ROWS:]
        if state is not None:
            fade = jnp.exp(state[0] - highest)
            total = total + state[1] * fade
            read = read + state[2] * fade
        return highest, total, read

    project(tp, 0, steps)
    state = attend(None, tp, 0, steps)
    near.wait_recv()
    project(partner, 0, steps)
    state = attend(state, partner, 0, steps)

    forwards = []
    for j in range(steps):
        for d in range(1, chips):
            source = lax.rem(tp + n_tp - 2 * d, n_tp)
            other = source + 1 - 2 * lax.rem(source, 2)
            far[d, j].wait_recv()
            forward = pltpu.make_async_remote_copy(
                src_ref=xg.at[source, pl.ds(j * chunk, chunk)],
                dst_ref=xg.at[source, pl.ds(j * chunk, chunk)],
                send_sem=fwd_send.at[d - 1, j],
                recv_sem=fwd_recv.at[d - 1, j],
                device_id={"tp": partner},
                device_id_type=MESH,
            )
            forward.start()
            forwards.append(forward)
            project(source, j, 1)
            state = attend(state, source, j, 1)
            forward.wait_recv()
            project(other, j, 1)
            state = attend(state, other, j, 1)

    for load in loads[6:]:
        load.wait()
    highest, total, read = state
    head_of = lax.broadcasted_iota(jnp.int32, (MAP_ROWS, wide), 0) // 2
    own = jnp.zeros((MAP_ROWS, wide), jnp.float32)
    for h in range(heads):
        own = jnp.where(head_of == h, read[:, h * wide:(h + 1) * wide], own)
    first_lane = lax.broadcasted_iota(jnp.int32, (MAP_ROWS, wide), 1) == 0
    stats[sp, 0] = own[:maps]
    stats[sp, 1] = jnp.where(first_lane, highest, total)[:maps]

    exchanges = []
    for d in range(n_sp - 1, 0, -1):
        copy = pltpu.make_async_remote_copy(
            src_ref=stats.at[sp],
            dst_ref=stats.at[sp],
            send_sem=st_send.at[d - 1],
            recv_sem=st_recv.at[d - 1],
            device_id={"sp": lax.rem(sp + d, n_sp)},
            device_id_type=MESH,
        )
        copy.start()
        exchanges.append(copy)
    for copy in exchanges:
        copy.wait_recv()
    heights = stats[:, 1]
    tops = heights[:, :, 0:1]
    sums = heights[:, :, 1:2]
    factor = jnp.exp(tops - jnp.max(tops, axis=0, keepdims=True))
    totals = jnp.sum(sums * factor, axis=0)
    reads = jnp.sum(stats[:, 0] * factor, axis=0) / totals
    normed = []
    for h in range(heads):
        diff = reads[2 * h:2 * h + 1] - lam[0:1, h:h + 1] * reads[2 * h + 1:2 * h + 2]
        scale = lax.rsqrt(jnp.mean(diff * diff, axis=1, keepdims=True) + 1e-06)
        normed.append(diff * scale * gain[...])
    headed = jnp.concatenate(normed, axis=1)
    headed = jnp.broadcast_to(headed, (MAP_ROWS, headed.shape[1])).astype(jnp.bfloat16)
    partials = jnp.dot(headed, wo[...], preferred_element_type=jnp.float32).astype(jnp.bfloat16)
    for b in range(n_tp):
        part[b] = partials[:, b * out_cols:(b + 1) * out_cols]
    swaps = []
    for d in range(n_tp - 1, 0, -1):
        target = lax.rem(tp + d, n_tp)
        copy = pltpu.make_async_remote_copy(
            src_ref=part.at[target],
            dst_ref=parts.at[d - 1],
            send_sem=pt_send.at[d - 1],
            recv_sem=pt_recv.at[d - 1],
            device_id={"tp": target},
            device_id_type=MESH,
        )
        copy.start()
        swaps.append(copy)
    mixed = part[tp].astype(jnp.float32)
    for copy in swaps:
        copy.wait_recv()
    for d in range(1, n_tp):
        mixed = mixed + parts[d - 1].astype(jnp.float32)
    mix_ref[...] = mixed[0:1].astype(jnp.bfloat16)

    near.wait_send()
    for copy in list(far.values()) + forwards + exchanges + swaps:
        copy.wait_send()


def tables(length, chunk, head_dim):
    inverse = 1.0 / 10000.0 ** (np.arange(0, head_dim, 2) / head_dim)
    inverse = np.tile(inverse, 4)
    sign = np.tile(np.repeat([-1.0, 1.0], head_dim // 2), 2)

    def pair(positions, axis):
        angles = positions[:, None] * inverse[None, :]
        both = np.stack([np.cos(angles), np.sin(angles) * sign], axis=axis)
        return both.astype(np.float32)

    return pair(np.arange(chunk), 0), pair(np.arange(0, length, chunk), 1)


def on_device(n_sp, n_tp, x, key_weight, value_weight, new_queries, lambdas, head_gain, out_weight):
    heads = lambdas.shape[0]
    columns = key_weight.shape[1]
    head_dim = columns // (2 * heads)
    wide = 2 * head_dim
    seqs, rows, depth = x.shape
    assert seqs == 1
    chunk = rows // 4
    steps = rows // chunk
    chips = n_tp // 2
    out_cols = out_weight.shape[1] // n_tp
    fine, coarse = tables(n_sp * n_tp * rows, chunk, head_dim)
    hbm_spec = pl.BlockSpec(memory_space=pltpu.HBM)
    dma = pltpu.SemaphoreType.DMA
    bf16 = jnp.bfloat16
    f32 = jnp.float32
    room = 2 * n_tp * rows * columns * 2 + SMALL_BYTES
    k, v, mixed = pl.pallas_call(
        functools.partial(kernel, n_sp, n_tp, heads, head_dim, chunk),
        out_shape=(
            pltpu.VMEM((n_tp, rows, columns), bf16),
            pltpu.VMEM((n_tp, rows, columns), bf16),
            jax.ShapeDtypeStruct((1, out_cols), bf16),
        ),
        in_specs=[hbm_spec] * 9,
        out_specs=(pl.BlockSpec(memory_space=pltpu.VMEM),) * 3,
        scratch_shapes=[
            pltpu.VMEM((n_tp, rows, depth), bf16),
            pltpu.VMEM((depth, columns), bf16),
            pltpu.VMEM((depth, columns), bf16),
            pltpu.VMEM(out_weight.shape, bf16),
            pltpu.VMEM((1, columns), bf16),
            pltpu.VMEM((1, heads), f32),
            pltpu.VMEM((1, wide), f32),
            pltpu.VMEM((2, chunk, wide), f32),
            pltpu.VMEM((n_tp * steps, 2, wide), f32),
            pltpu.VMEM((n_sp, 2, 2 * heads, wide), f32),
            pltpu.VMEM((n_tp, MAP_ROWS, out_cols), bf16),
            pltpu.VMEM((n_tp - 1, MAP_ROWS, out_cols), bf16),
            dma((9,)),
            pltpu.SemaphoreType.REGULAR,
            pltpu.SemaphoreType.REGULAR,
            dma,
            dma,
            dma((chips - 1, steps)),
            dma((chips - 1, steps)),
            dma((chips - 1, steps)),
            dma((chips - 1, steps)),
            dma((n_sp - 1,)),
            dma((n_sp - 1,)),
            dma((n_tp - 1,)),
            dma((n_tp - 1,)),
        ],
        compiler_params=pltpu.CompilerParams(
            collective_id=0, has_side_effects=True, vmem_limit_bytes=VMEM_BYTES - room
        ),
    )(
        x, key_weight, value_weight, new_queries, lambdas.reshape(1, heads),
        head_gain.reshape(1, wide), out_weight, jnp.asarray(fine), jnp.asarray(coarse),
    )
    full = (1, n_tp * rows, columns)
    return k.reshape(full), v.reshape(full), mixed


def solution(mesh):
    n_sp, n_tp = mesh.shape["sp"], mesh.shape["tp"]
    in_specs = (
        P("gr", ("sp", "tp"), None),
        P(None, "tp"),
        P(None, "tp"),
        P("gr", "tp"),
        P("tp"),
        P(),
        P("tp", None),
    )
    out_specs = (P("gr", "sp", "tp"), P("gr", "sp", "tp"), P("gr", "tp"))
    return jax.shard_map(
        functools.partial(on_device, n_sp, n_tp),
        mesh=mesh, in_specs=in_specs, out_specs=out_specs, check_vma=False,
    )
```

```python
import functools

import jax
import jax.numpy as jnp
import numpy as np
from jax import lax
from jax.experimental import pallas as pl
from jax.experimental.pallas import tpu as pltpu
from jax.sharding import PartitionSpec as P

MESH = pl.DeviceIdType.MESH
MAP_ROWS = 16
VMEM_BYTES = 67043328
SMALL_BYTES = 16384


def kernel(
    n_sp, n_tp, heads, head_dim, chunk,
    x_ref, wk_ref, wv_ref, q_ref, lam_ref, gain_ref, wo_ref, fine_ref, coarse_ref,
    keys, values, mix_ref,
    xg, wk, wv, wo, q, lam, gain, fine, coarse, stats, part, parts,
    load_sem, up_sem, down_sem, near_send, near_recv, far_send, far_recv, fwd_send, fwd_recv,
    st_send, st_recv, pt_send, pt_recv,
):
    sp = lax.axis_index("sp")
    tp = lax.axis_index("tp")
    rows = x_ref.shape[1]
    wide = 2 * head_dim
    maps = 2 * heads
    steps = rows // chunk
    chips = n_tp // 2
    partner = tp + 1 - 2 * lax.rem(tp, 2)
    out_cols = mix_ref.shape[1]
    local_coarse = n_tp * steps

    own_load = pltpu.make_async_copy(x_ref.at[0], xg.at[tp], load_sem.at[0])
    loads = [
        pltpu.make_async_copy(q_ref, q, load_sem.at[5]),
        pltpu.make_async_copy(wk_ref, wk, load_sem.at[1]),
        pltpu.make_async_copy(wv_ref, wv, load_sem.at[2]),
        pltpu.make_async_copy(fine_ref, fine, load_sem.at[3]),
        pltpu.make_async_copy(
            coarse_ref.at[pl.ds(sp * local_coarse, local_coarse)], coarse, load_sem.at[4]
        ),
        pltpu.make_async_copy(lam_ref, lam, load_sem.at[6]),
        pltpu.make_async_copy(gain_ref, gain, load_sem.at[7]),
        pltpu.make_async_copy(wo_ref, wo, load_sem.at[8]),
    ]

    own_load.start()
    barrier = pltpu.get_barrier_semaphore()
    for d in range(1, n_tp):
        pl.semaphore_signal(
            barrier, inc=1, device_id={"tp": lax.rem(tp + d, n_tp)}, device_id_type=MESH
        )
    has_lower = sp > 0
    has_upper = sp < n_sp - 1

    @pl.when(has_lower)
    def _():
        pl.semaphore_signal(barrier, inc=1, device_id={"sp": sp - 1}, device_id_type=MESH)

    @pl.when(has_upper)
    def _():
        pl.semaphore_signal(barrier, inc=1, device_id={"sp": sp + 1}, device_id_type=MESH)

    pl.semaphore_wait(barrier, n_tp - 1 + jnp.where(has_lower, 1, 0) + jnp.where(has_upper, 1, 0))

    own_load.wait()
    far = {}
    for j in range(steps):
        for d in range(1, chips):
            far[d, j] = pltpu.make_async_remote_copy(
                src_ref=xg.at[tp, pl.ds(j * chunk, chunk)],
                dst_ref=xg.at[tp, pl.ds(j * chunk, chunk)],
                send_sem=far_send.at[d - 1, j],
                recv_sem=far_recv.at[d - 1, j],
                device_id={"tp": lax.rem(tp + 2 * d, n_tp)},
                device_id_type=MESH,
            )
            far[d, j].start()
    near = pltpu.make_async_remote_copy(
        src_ref=xg.at[tp],
        dst_ref=xg.at[tp],
        send_sem=near_send,
        recv_sem=near_recv,
        device_id={"tp": partner},
        device_id_type=MESH,
    )
    for load in loads:
        load.start()
    near.start()

    pl.when(has_lower)(lambda: pl.semaphore_wait(up_sem, 1))

    @pl.when(has_upper)
    def _():
        pl.semaphore_signal(up_sem, inc=1, device_id={"sp": sp + 1}, device_id_type=MESH)
        pl.semaphore_wait(down_sem, 1)

    @pl.when(has_lower)
    def _():
        pl.semaphore_signal(down_sem, inc=1, device_id={"sp": sp - 1}, device_id_type=MESH)

    lane = lax.broadcasted_iota(jnp.int32, (chunk, wide), 1)
    low_half = lax.rem(lane, head_dim) < head_dim // 2

    def project(block, first, count):
        piece = xg[block, first * chunk:(first + count) * chunk, :]
        raw_keys = jnp.dot(piece, wk[...], preferred_element_type=jnp.float32)
        raw_values = jnp.dot(piece, wv[...], preferred_element_type=jnp.float32)
        values[block, first * chunk:(first + count) * chunk, :] = raw_values.astype(jnp.bfloat16)
        for i in range(count):
            base = coarse[block * steps + first + i]
            base_cos, base_sin = base[0:1, :], base[1:2, :]
            cosine = base_cos * fine[0] - base_sin * fine[1]
            sine = base_sin * fine[0] + base_cos * fine[1]
            for h in range(heads):
                raw = raw_keys[i * chunk:(i + 1) * chunk, h * wide:(h + 1) * wide]
                ahead = pltpu.roll(raw, wide - head_dim // 2, 1)
                behind = pltpu.roll(raw, head_dim // 2, 1)
                turned = raw * cosine + jnp.where(low_half, ahead, behind) * sine
                keys[
                    block, (first + i) * chunk:(first + i + 1) * chunk, h * wide:(h + 1) * wide
                ] = turned.astype(jnp.bfloat16)

    for load in loads[:5]:
        load.wait()
    map_row = lax.broadcasted_iota(jnp.int32, (MAP_ROWS, q.shape[1]), 0)
    map_col = lax.broadcasted_iota(jnp.int32, (MAP_ROWS, q.shape[1]), 1) // head_dim
    spread = jnp.where(map_row == map_col, q[...].astype(jnp.float32), 0.0).astype(jnp.bfloat16)

    def attend(state, block, first, count):
        where = slice(first * chunk, (first + count) * chunk)
        score = lax.dot_general(
            spread, keys[block, where, :], (((1,), (1,)), ((), ())),
            preferred_element_type=jnp.float32,
        ) * head_dim ** (-0.5)
        highest = jnp.max(score, axis=1, keepdims=True)
        if state is not None:
            highest = jnp.maximum(highest, state[0])
        weight = jnp.exp(score - highest)
        total = jnp.sum(weight, axis=1, keepdims=True)
        upper = weight.astype(jnp.bfloat16)
        lower = (weight - upper.astype(jnp.float32)).astype(jnp.bfloat16)
        read = jnp.dot(
            jnp.concatenate([upper, lower], axis=0), values[block, where, :],
            preferred_element_type=jnp.float32,
        )
        read = read[:MAP_ROWS] + read[MAP_ROWS:]
        if state is not None:
            fade = jnp.exp(state[0] - highest)
            total = total + state[1] * fade
            read = read + state[2] * fade
        return highest, total, read

    project(tp, 0, steps)
    state = attend(None, tp, 0, steps)
    near.wait_recv()
    project(partner, 0, steps)
    state = attend(state, partner, 0, steps)

    forwards = []
    for j in range(steps):
        for d in range(1, chips):
            source = lax.rem(tp + n_tp - 2 * d, n_tp)
            other = source + 1 - 2 * lax.rem(source, 2)
            far[d, j].wait_recv()
            forward = pltpu.make_async_remote_copy(
                src_ref=xg.at[source, pl.ds(j * chunk, chunk)],
                dst_ref=xg.at[source, pl.ds(j * chunk, chunk)],
                send_sem=fwd_send.at[d - 1, j],
                recv_sem=fwd_recv.at[d - 1, j],
                device_id={"tp": partner},
                device_id_type=MESH,
            )
            forward.start()
            forwards.append(forward)
            project(source, j, 1)
            state = attend(state, source, j, 1)
            forward.wait_recv()
            project(other, j, 1)
            state = attend(state, other, j, 1)

    for load in loads[5:]:
        load.wait()
    highest, total, read = state
    head_of = lax.broadcasted_iota(jnp.int32, (MAP_ROWS, wide), 0) // 2
    own = jnp.zeros((MAP_ROWS, wide), jnp.float32)
    for h in range(heads):
        own = jnp.where(head_of == h, read[:, h * wide:(h + 1) * wide], own)
    first_lane = lax.broadcasted_iota(jnp.int32, (MAP_ROWS, wide), 1) == 0
    stats[sp, 0] = own[:maps]
    stats[sp, 1] = jnp.where(first_lane, highest, total)[:maps]

    exchanges = []
    for d in range(n_sp - 1, 0, -1):
        copy = pltpu.make_async_remote_copy(
            src_ref=stats.at[sp],
            dst_ref=stats.at[sp],
            send_sem=st_send.at[d - 1],
            recv_sem=st_recv.at[d - 1],
            device_id={"sp": lax.rem(sp + d, n_sp)},
            device_id_type=MESH,
        )
        copy.start()
        exchanges.append(copy)
    for copy in exchanges:
        copy.wait_recv()
    heights = stats[:, 1]
    tops = heights[:, :, 0:1]
    sums = heights[:, :, 1:2]
    factor = jnp.exp(tops - jnp.max(tops, axis=0, keepdims=True))
    totals = jnp.sum(sums * factor, axis=0)
    reads = jnp.sum(stats[:, 0] * factor, axis=0) / totals
    normed = []
    for h in range(heads):
        diff = reads[2 * h:2 * h + 1] - lam[0:1, h:h + 1] * reads[2 * h + 1:2 * h + 2]
        scale = lax.rsqrt(jnp.mean(diff * diff, axis=1, keepdims=True) + 1e-06)
        normed.append(diff * scale * gain[...])
    headed = jnp.concatenate(normed, axis=1)
    headed = jnp.broadcast_to(headed, (MAP_ROWS, headed.shape[1])).astype(jnp.bfloat16)
    partials = jnp.dot(headed, wo[...], preferred_element_type=jnp.float32).astype(jnp.bfloat16)
    for b in range(n_tp):
        part[b] = partials[:, b * out_cols:(b + 1) * out_cols]
    swaps = []
    for d in range(n_tp - 1, 0, -1):
        target = lax.rem(tp + d, n_tp)
        copy = pltpu.make_async_remote_copy(
            src_ref=part.at[target],
            dst_ref=parts.at[d - 1],
            send_sem=pt_send.at[d - 1],
            recv_sem=pt_recv.at[d - 1],
            device_id={"tp": target},
            device_id_type=MESH,
        )
        copy.start()
        swaps.append(copy)
    mixed = part[tp].astype(jnp.float32)
    for copy in swaps:
        copy.wait_recv()
    for d in range(1, n_tp):
        mixed = mixed + parts[d - 1].astype(jnp.float32)
    mix_ref[...] = mixed[0:1].astype(jnp.bfloat16)

    near.wait_send()
    for copy in list(far.values()) + forwards + exchanges + swaps:
        copy.wait_send()


def tables(length, chunk, head_dim):
    inverse = 1.0 / 10000.0 ** (np.arange(0, head_dim, 2) / head_dim)
    inverse = np.tile(inverse, 4)
    sign = np.tile(np.repeat([-1.0, 1.0], head_dim // 2), 2)

    def pair(positions, axis):
        angles = positions[:, None] * inverse[None, :]
        both = np.stack([np.cos(angles), np.sin(angles) * sign], axis=axis)
        return both.astype(np.float32)

    return pair(np.arange(chunk), 0), pair(np.arange(0, length, chunk), 1)


def on_device(n_sp, n_tp, x, key_weight, value_weight, new_queries, lambdas, head_gain, out_weight):
    heads = lambdas.shape[0]
    columns = key_weight.shape[1]
    head_dim = columns // (2 * heads)
    wide = 2 * head_dim
    seqs, rows, depth = x.shape
    assert seqs == 1
    chunk = rows // 4
    steps = rows // chunk
    chips = n_tp // 2
    out_cols = out_weight.shape[1] // n_tp
    fine, coarse = tables(n_sp * n_tp * rows, chunk, head_dim)
    hbm_spec = pl.BlockSpec(memory_space=pltpu.HBM)
    dma = pltpu.SemaphoreType.DMA
    bf16 = jnp.bfloat16
    f32 = jnp.float32
    room = 2 * n_tp * rows * columns * 2 + SMALL_BYTES
    k, v, mixed = pl.pallas_call(
        functools.partial(kernel, n_sp, n_tp, heads, head_dim, chunk),
        out_shape=(
            pltpu.VMEM((n_tp, rows, columns), bf16),
            pltpu.VMEM((n_tp, rows, columns), bf16),
            jax.ShapeDtypeStruct((1, out_cols), bf16),
        ),
        in_specs=[hbm_spec] * 9,
        out_specs=(pl.BlockSpec(memory_space=pltpu.VMEM),) * 3,
        scratch_shapes=[
            pltpu.VMEM((n_tp, rows, depth), bf16),
            pltpu.VMEM((depth, columns), bf16),
            pltpu.VMEM((depth, columns), bf16),
            pltpu.VMEM(out_weight.shape, bf16),
            pltpu.VMEM((1, columns), bf16),
            pltpu.VMEM((1, heads), f32),
            pltpu.VMEM((1, wide), f32),
            pltpu.VMEM((2, chunk, wide), f32),
            pltpu.VMEM((n_tp * steps, 2, wide), f32),
            pltpu.VMEM((n_sp, 2, 2 * heads, wide), f32),
            pltpu.VMEM((n_tp, MAP_ROWS, out_cols), bf16),
            pltpu.VMEM((n_tp - 1, MAP_ROWS, out_cols), bf16),
            dma((9,)),
            pltpu.SemaphoreType.REGULAR,
            pltpu.SemaphoreType.REGULAR,
            dma,
            dma,
            dma((chips - 1, steps)),
            dma((chips - 1, steps)),
            dma((chips - 1, steps)),
            dma((chips - 1, steps)),
            dma((n_sp - 1,)),
            dma((n_sp - 1,)),
            dma((n_tp - 1,)),
            dma((n_tp - 1,)),
        ],
        compiler_params=pltpu.CompilerParams(
            collective_id=0, has_side_effects=True, vmem_limit_bytes=VMEM_BYTES - room
        ),
    )(
        x, key_weight, value_weight, new_queries, lambdas.reshape(1, heads),
        head_gain.reshape(1, wide), out_weight, jnp.asarray(fine), jnp.asarray(coarse),
    )
    full = (1, n_tp * rows, columns)
    return k.reshape(full), v.reshape(full), mixed


def solution(mesh):
    n_sp, n_tp = mesh.shape["sp"], mesh.shape["tp"]
    in_specs = (
        P("gr", ("sp", "tp"), None),
        P(None, "tp"),
        P(None, "tp"),
        P("gr", "tp"),
        P("tp"),
        P(),
        P("tp", None),
    )
    out_specs = (P("gr", "sp", "tp"), P("gr", "sp", "tp"), P("gr", "tp"))
    return jax.shard_map(
        functools.partial(on_device, n_sp, n_tp),
        mesh=mesh, in_specs=in_specs, out_specs=out_specs, check_vma=False,
    )
```
